32 devices in a mesh: kv: 16 (over z, y, x), tp: 2 (over core).
Axes of the slice: x: 2, y: 2, z: 4, core: 2. Of those that a mesh axis runs over, the one named last changes fastest.
Arguments:
- tokens: bfloat16 [24, 4096], P(None, 'kv'), may hold values from -60 to 60
- gain_first: bfloat16 [4096], P('kv'), may hold values from 0.099609375 to 1.8984375
- gate_first: bfloat16 [4096, 11264], P('kv', 'tp'), may hold values from -0.09375 to 0.09375
- up_first: bfloat16 [4096, 11264], P('kv', 'tp'), may hold values from -0.09375 to 0.09375
- down_first: bfloat16 [11264, 4096], P('tp', 'kv'), may hold values from -0.0546875 to 0.0546875
- gain_mixer: bfloat16 [4096], P('kv'), may hold values from 0.099609375 to 1.8984375
- query_weight: bfloat16 [4096, 2048], P('kv', 'tp'), may hold values from -0.09375 to 0.09375
- key_weight: bfloat16 [4096, 2048], P('kv', 'tp'), may hold values from -0.25 to 0.25
- value_weight: bfloat16 [4096, 2048], P('kv', 'tp'), may hold values from -0.09375 to 0.09375
- forget_weight: bfloat16 [4096, 16], replicated, may hold values from -0.09375 to 0.09375
- forget_bias: float32 [16], replicated, may hold values from -1 to 2
- key_cache: bfloat16 [24, 8192, 16, 128], P(None, 'kv', 'tp'), may hold values from -2000 to 2000
- value_cache: bfloat16 [24, 8192, 16, 128], P(None, 'kv', 'tp'), may hold values from -6 to 6
- forget_sum: float32 [24, 16, 8192], P(None, 'tp', 'kv'), may hold values from -1024 to 0, as said below
- out_weight: bfloat16 [2048, 4096], P('tp', 'kv'), may hold values from -0.5 to 0.5
- gain_second: bfloat16 [4096], P('kv'), may hold values from 0.099609375 to 1.8984375
- gate_second: bfloat16 [4096, 11264], P('kv', 'tp'), may hold values from -0.09375 to 0.09375
- up_second: bfloat16 [4096, 11264], P('kv', 'tp'), may hold values from -0.09375 to 0.09375
- down_second: bfloat16 [11264, 4096], P('tp', 'kv'), may hold values from -0.0546875 to 0.0546875
Outputs:
- updated: bfloat16 [24, 4096], P(None, 'kv')
The draws below stay inside these ranges and needn't reach their ends.
Inputs may be any that keep to these rules, and one draw needn't show every extreme that they name: forget_sum[b, h, s] is the sum of the log forget gates of the cached positions after s, up to the last cached one, for sequence b and head h; it never falls with s, is at most 0, and rises to 0 at the last cached position.
All inputs are finite; a program needn't handle non-finite values.
Results may differ from the reference program's by a relative error of at most 0.02.
Values may be sent and summed in bfloat16 or wider, within the bound.
A program may use at most 128 MiB of HBM per device.

```python
import math
import jax
import jax.numpy as jnp
from jax import lax

D = 4096
HEAD_TOTAL = 16
HEAD_DIM = 128
FF = 11264
BLOCK = 128
SEQUENCE_TOTAL = 24
CACHE_LENGTH = 8192
N_KV = 16
N_TP = 2


def draw_tokens(key, part):
    random_subkeys = jax.random.split(jax.random.fold_in(key, 11), 4)
    row_scale = jnp.exp(jax.random.uniform(random_subkeys[0], (SEQUENCE_TOTAL, 1), jnp.float32, math.log(0.3), math.log(3.0)))
    column_ramp = jnp.exp(jnp.linspace(0.0, math.log(3.0), D, dtype=jnp.float32))[None, :]
    roughness = jax.random.uniform(random_subkeys[1], (1, D), jnp.float32, 0.5, 1.5)
    values = jax.random.normal(random_subkeys[3], (SEQUENCE_TOTAL, D), jnp.float32) * row_scale * column_ramp * roughness
    return jnp.clip(values, -60.0, 60.0).astype(jnp.bfloat16)


def draw_key_cache(key, part):
    random_subkeys = jax.random.split(jax.random.fold_in(key, 17), 6)
    cache_shape = (SEQUENCE_TOTAL, CACHE_LENGTH, HEAD_TOTAL, HEAD_DIM)
    base_keys = jax.random.normal(random_subkeys[0], cache_shape, jnp.float32)
    chosen = jax.random.uniform(random_subkeys[1], (SEQUENCE_TOTAL, 1, HEAD_TOTAL, 1), jnp.float32) < 0.5
    strength = jnp.exp(jax.random.uniform(random_subkeys[2], (SEQUENCE_TOTAL, 1, HEAD_TOTAL, 1), jnp.float32, math.log(40.0), math.log(300.0)))
    first_spot = jax.random.randint(random_subkeys[3], (SEQUENCE_TOTAL, 1, HEAD_TOTAL, 1), 0, CACHE_LENGTH - 1)
    cache_position = jnp.arange(CACHE_LENGTH, dtype=jnp.int32).reshape(1, CACHE_LENGTH, 1, 1)
    direction = jax.random.normal(random_subkeys[4], (SEQUENCE_TOTAL, 1, HEAD_TOTAL, HEAD_DIM), jnp.float32)
    nudge_dir = jax.random.normal(random_subkeys[5], (SEQUENCE_TOTAL, 1, HEAD_TOTAL, HEAD_DIM), jnp.float32)
    planted = jnp.where(cache_position == first_spot, strength * direction, base_keys)
    planted = jnp.where(cache_position == first_spot + 1, strength * direction + 1.5 * nudge_dir, planted)
    base_keys = jnp.where(chosen, planted, base_keys)
    return jnp.clip(base_keys, -2000.0, 2000.0).astype(jnp.bfloat16)


def draw_forget_sum(key, part):
    random_subkeys = jax.random.split(jax.random.fold_in(key, 23), 7)
    slow_share = 0.5
    slow_flag = jax.random.uniform(random_subkeys[0], (SEQUENCE_TOTAL, HEAD_TOTAL, 1), jnp.float32) < slow_share
    slow_total = jnp.exp(jax.random.uniform(random_subkeys[1], (SEQUENCE_TOTAL, HEAD_TOTAL, 1), jnp.float32, math.log(0.7), math.log(2.5)))
    fast_rate = jnp.exp(jax.random.uniform(random_subkeys[2], (SEQUENCE_TOTAL, HEAD_TOTAL, 1), jnp.float32, math.log(0.01), math.log(1.0 / 30.0)))
    decay_rate = jnp.where(slow_flag, slow_total / CACHE_LENGTH, fast_rate)
    device_factor = jnp.exp(jax.random.uniform(random_subkeys[3], (SEQUENCE_TOTAL, HEAD_TOTAL, N_KV), jnp.float32, math.log(0.5), math.log(2.0)))
    device_factor = jnp.repeat(device_factor, CACHE_LENGTH // N_KV, axis=2)
    roughness = jax.random.uniform(random_subkeys[4], (SEQUENCE_TOTAL, HEAD_TOTAL, CACHE_LENGTH), jnp.float32, 0.5, 1.5)
    descent_steps = -decay_rate * device_factor * roughness
    spike_location = jax.random.randint(random_subkeys[5], (SEQUENCE_TOTAL, HEAD_TOTAL, 3), 0, CACHE_LENGTH)
    spike_depth = jnp.log(jax.random.uniform(random_subkeys[6], (SEQUENCE_TOTAL, HEAD_TOTAL, 3), jnp.float32, 0.5, 0.8))
    cache_position = jnp.arange(CACHE_LENGTH, dtype=jnp.int32)
    spike_list = jnp.sum(jnp.where(cache_position[None, None, None, :] == spike_location[..., None], spike_depth[..., None], 0.0), axis=2)
    descent_steps = descent_steps + jnp.where(slow_flag, spike_list, 0.0)
    running = jnp.cumsum(descent_steps, axis=2)
    return running[:, :, -1:] - running


def block_scale(own_key, dims, cuts, low, top_value):
    factor_of = 1.0
    for axis_at, parts in cuts:
        heights = jax.random.uniform(jax.random.fold_in(jax.random.fold_in(own_key, 6), axis_at), (parts,), jnp.float32, low / len(cuts), top_value / len(cuts))
        factor_of = factor_of * jnp.repeat(jnp.exp(heights), dims[axis_at] // parts).reshape((-1,) + (1,) * (len(dims) - 1 - axis_at))
    return factor_of


def scatter_about(rng, extent, deviation, most, cuts=(), kind=jnp.bfloat16):
    gain = block_scale(rng, extent, cuts, -0.22, 0.18) if cuts else 1.0
    result = jax.random.normal(rng, extent, jnp.float32) * deviation * gain
    return jnp.minimum(jnp.maximum(result, -most), most).astype(kind)


def setup_inputs(seed: int = 0) -> dict:
    keys = jax.random.split(jax.random.key(seed), 20)
    tokens = draw_tokens(jax.random.fold_in(keys[19], 71), 0)
    gain_first = jnp.clip(1.0 + 0.18 * jax.random.normal(keys[1], (D,), jnp.float32), 0.099609375, 1.8984375).astype(jnp.bfloat16)
    gate_first = scatter_about(keys[2], (D, FF), D ** -0.5, 0.09375, ((0, 16), (1, 2)))
    up_first = scatter_about(keys[3], (D, FF), D ** -0.5, 0.09375, ((0, 16), (1, 2)))
    down_first = scatter_about(keys[4], (FF, D), FF ** -0.5, 0.0546875, ((0, 2), (1, 16)))
    gain_mixer = jnp.clip(1.0 + 0.18 * jax.random.normal(keys[5], (D,), jnp.float32), 0.099609375, 1.8984375).astype(jnp.bfloat16)
    query_weight = scatter_about(keys[6], (D, HEAD_TOTAL * HEAD_DIM), D ** -0.5, 0.09375, ((0, 16), (1, 2)))
    key_weight = scatter_about(keys[7], (D, HEAD_TOTAL * HEAD_DIM), (D // 8) ** -0.5, 0.25, ((0, 16), (1, 2)))
    value_weight = scatter_about(keys[8], (D, HEAD_TOTAL * HEAD_DIM), D ** -0.5, 0.09375, ((0, 16), (1, 2)))
    forget_weight = scatter_about(keys[9], (D, HEAD_TOTAL), D ** -0.5, 0.09375)
    forget_bias = jnp.clip(jax.random.uniform(keys[10], (HEAD_TOTAL,), jnp.float32, -1.0, 2.0), -1.0, 2.0)
    key_cache = draw_key_cache(jax.random.fold_in(keys[19], 71), 0)
    value_cache = scatter_about(keys[12], (SEQUENCE_TOTAL, CACHE_LENGTH, HEAD_TOTAL, HEAD_DIM), 1.0, 6.0, ((1, 16), (2, 2)))
    forget_sum = draw_forget_sum(jax.random.fold_in(keys[19], 71), 0)
    out_weight = scatter_about(keys[14], (HEAD_TOTAL * HEAD_DIM, D), (HEAD_TOTAL * HEAD_DIM // 16) ** -0.5, 0.5, ((0, 2), (1, 16)))
    gain_second = jnp.clip(1.0 + 0.18 * jax.random.normal(keys[15], (D,), jnp.float32), 0.099609375, 1.8984375).astype(jnp.bfloat16)
    gate_second = scatter_about(keys[16], (D, FF), D ** -0.5, 0.09375, ((0, 16), (1, 2)))
    up_second = scatter_about(keys[17], (D, FF), D ** -0.5, 0.09375, ((0, 16), (1, 2)))
    down_second = scatter_about(keys[18], (FF, D), FF ** -0.5, 0.0546875, ((0, 2), (1, 16)))
    return dict(tokens=tokens, gain_first=gain_first, gate_first=gate_first, up_first=up_first, down_first=down_first, gain_mixer=gain_mixer, query_weight=query_weight, key_weight=key_weight, value_weight=value_weight, forget_weight=forget_weight, forget_bias=forget_bias, key_cache=key_cache, value_cache=value_cache, forget_sum=forget_sum, out_weight=out_weight, gain_second=gain_second, gate_second=gate_second, up_second=up_second, down_second=down_second)


EPSILON = 1e-06

def row_factor(tokens):
    widened = tokens.astype(jnp.float32)
    return lax.rsqrt(lax.optimization_barrier(jnp.mean(widened * widened, axis=1, keepdims=True)) + EPSILON)

def scaled_rows(tokens, norm_gain):
    return (tokens.astype(jnp.float32) * norm_gain.astype(jnp.float32)).astype(jnp.bfloat16)

def grouped_sum(left, right, groups):
    seq_count = left.shape[0]
    left_groups = left.reshape(seq_count, groups, -1).astype(jnp.float32)
    right_groups = right.reshape(groups, -1, right.shape[1]).astype(jnp.float32)
    partial_value = jnp.einsum('bgf,gfd->gbd', left_groups, right_groups).astype(jnp.bfloat16)
    partial_value = lax.optimization_barrier(partial_value)
    return lax.optimization_barrier(jnp.sum(partial_value.astype(jnp.float32), axis=0))

def feed_forward(tokens, norm_gain, gate_matrix, up_matrix, down_matrix):
    factor = row_factor(tokens)
    scaled = scaled_rows(tokens, norm_gain)
    gate_value = factor * jnp.dot(scaled, gate_matrix, preferred_element_type=jnp.float32)
    up_value = factor * jnp.dot(scaled, up_matrix, preferred_element_type=jnp.float32)
    hidden = (jax.nn.silu(gate_value) * up_value).astype(jnp.bfloat16)
    summed = grouped_sum(hidden, down_matrix, N_TP)
    return (tokens.astype(jnp.float32) + 0.5 * summed).astype(jnp.bfloat16)

def attend_one(items):
    query_rows, new_key, new_value, log_gate, cached_keys, cached_values, forget_row = items
    inverse = query_rows.shape[1] ** (-0.5)
    scores = jnp.einsum('hd,lhd->hl', query_rows.astype(jnp.float32), cached_keys.astype(jnp.float32)) * inverse
    scores = scores + forget_row + log_gate[:, None]
    head_count = scores.shape[0]
    blocks = scores.shape[1] // BLOCK
    scores = scores.reshape(head_count, blocks, BLOCK)
    highest = lax.optimization_barrier(jnp.max(scores, axis=2))
    weights = jnp.exp(scores - highest[..., None]).astype(jnp.bfloat16)
    block_sum = lax.optimization_barrier(jnp.sum(weights.astype(jnp.float32), axis=2))
    block_value = jnp.einsum('hcs,cshd->hcd', weights.astype(jnp.float32), cached_values.reshape(blocks, BLOCK, head_count, -1).astype(jnp.float32))
    own_score = lax.optimization_barrier(jnp.sum(query_rows.astype(jnp.float32) * new_key.astype(jnp.float32), axis=1)) * inverse
    ceiling = jnp.maximum(lax.optimization_barrier(jnp.max(highest, axis=1)), own_score)
    cache_scale = jnp.exp(highest - ceiling[:, None])
    own_scale = jnp.exp(own_score - ceiling)
    numerator = lax.optimization_barrier(jnp.sum(cache_scale[..., None] * block_value, axis=1)) + own_scale[:, None] * new_value.astype(jnp.float32)
    denominator = lax.optimization_barrier(jnp.sum(cache_scale * block_sum, axis=1)) + own_scale
    return (numerator / denominator[:, None]).astype(jnp.bfloat16)

def mix_tokens(tokens, norm_gain, query_weight, key_weight, value_weight, forget_weight, forget_bias, key_cache, value_cache, forget_sum, out_weight):
    factor = row_factor(tokens)
    scaled = scaled_rows(tokens, norm_gain)
    seq_count = tokens.shape[0]
    head_count = key_cache.shape[2]

    def project(matrix):
        product = factor * jnp.dot(scaled, matrix, preferred_element_type=jnp.float32)
        return product.astype(jnp.bfloat16).reshape(seq_count, head_count, -1)
    query_rows = project(query_weight)
    new_key = project(key_weight)
    new_value = project(value_weight)
    log_gate = jax.nn.log_sigmoid(factor * jnp.dot(scaled, forget_weight, preferred_element_type=jnp.float32) + forget_bias)
    attended = lax.map(attend_one, (query_rows, new_key, new_value, log_gate, key_cache, value_cache, forget_sum))
    summed = grouped_sum(attended.reshape(seq_count, -1), out_weight, N_TP)
    return (tokens.astype(jnp.float32) + summed).astype(jnp.bfloat16)

def reference(tokens, gain_first, gate_first, up_first, down_first, gain_mixer, query_weight, key_weight, value_weight, forget_weight, forget_bias, key_cache, value_cache, forget_sum, out_weight, gain_second, gate_second, up_second, down_second):
    first_out = feed_forward(tokens, gain_first, gate_first, up_first, down_first)
    mixed = mix_tokens(first_out, gain_mixer, query_weight, key_weight, value_weight, forget_weight, forget_bias, key_cache, value_cache, forget_sum, out_weight)
    return feed_forward(mixed, gain_second, gate_second, up_second, down_second)
```

```python
import functools

import jax
import jax.numpy as jnp
from jax import lax
from jax.experimental import pallas as pl
from jax.experimental.pallas import tpu as pltpu
from jax.sharding import PartitionSpec as P

EPSILON = 1e-06
LANES = 128
F32 = jnp.float32
BF16 = jnp.bfloat16


def chunk_width(columns, devices):
    tiles = -(-columns // LANES)
    return LANES * (-(-tiles // devices))


def greet(n_kv, n_tp):
    me, core = lax.axis_index("kv"), lax.axis_index("tp")
    barrier = pltpu.get_barrier_semaphore()

    def along_kv(k, carry):
        pl.semaphore_signal(
            barrier, inc=1, device_id={"kv": lax.rem(me + k, n_kv)},
            device_id_type=pl.DeviceIdType.MESH,
        )
        return carry

    lax.fori_loop(1, n_kv, along_kv, 0)
    for k in range(1, n_tp):
        pl.semaphore_signal(
            barrier, inc=1, device_id={"tp": lax.rem(core + k, n_tp)},
            device_id_type=pl.DeviceIdType.MESH,
        )
    pl.semaphore_wait(barrier, n_kv - 1 + n_tp - 1)


def remote(source, target, send_sem, recv_sem, axis, peer):
    return pltpu.make_async_remote_copy(
        src_ref=source, dst_ref=target, send_sem=send_sem, recv_sem=recv_sem,
        device_id={axis: peer}, device_id_type=pl.DeviceIdType.MESH,
    )


def share(buffer, send_sems, recv_sems, axis, count):
    me = lax.axis_index(axis)

    def send(k, carry):
        peer = lax.rem(me + k, count)
        remote(buffer.at[me], buffer.at[me], send_sems.at[peer], recv_sems.at[me], axis, peer).start()
        return carry

    lax.fori_loop(1, count, send, 0)


def shared_from(buffer, send_sems, recv_sems, axis, peer):
    me = lax.axis_index(axis)
    remote(buffer.at[me], buffer.at[peer], send_sems.at[peer], recv_sems.at[peer], axis, peer).wait_recv()


def drain(buffer, send_sems, recv_sems, axis, count):
    me = lax.axis_index(axis)

    def done(k, carry):
        peer = lax.rem(me + k, count)
        remote(buffer.at[me], buffer.at[me], send_sems.at[peer], recv_sems.at[me], axis, peer).wait_send()
        return carry

    lax.fori_loop(1, count, done, 0)


def collect(buffer, send_sems, recv_sems, axis, count):
    me = lax.axis_index(axis)

    def arrived(k, carry):
        shared_from(buffer, send_sems, recv_sems, axis, lax.rem(me + k, count))
        return carry

    lax.fori_loop(1, count, arrived, 0)


def total_over(buffer, count):
    def add(j, so_far):
        return so_far + buffer[j].astype(F32)

    return lax.fori_loop(1, count, add, buffer[0].astype(F32))


def across_tp(part, tp_buf, send_sems, recv_sems, n_tp):
    tp_buf[lax.axis_index("tp")] = part.astype(BF16)
    share(tp_buf, send_sems, recv_sems, "tp", n_tp)
    collect(tp_buf, send_sems, recv_sems, "tp", n_tp)
    return total_over(tp_buf, n_tp)


def feed_kernel(
    n_kv, n_tp, width, d_total,
    tokens_ref, gain_ref, gate_hbm, up_hbm, down_hbm, out_ref,
    gate_v, up_v, down_v, stat, send, recv, hid, tp_buf,
    w_sems, stat_s, stat_r, rs_s, rs_r, ag_s, ag_r, tp_s, tp_r,
):
    me = lax.axis_index("kv")
    hidden_units = gate_hbm.shape[1]
    loads = [
        pltpu.make_async_copy(gate_hbm, gate_v.at[:, pl.ds(0, hidden_units)], w_sems.at[0]),
        pltpu.make_async_copy(up_hbm, up_v.at[:, pl.ds(0, hidden_units)], w_sems.at[1]),
        pltpu.make_async_copy(down_hbm, down_v.at[pl.ds(0, hidden_units)], w_sems.at[2]),
    ]
    for load in loads:
        load.start()
    padded = gate_v.shape[1]
    if padded > hidden_units:
        gate_v[:, hidden_units:] = jnp.zeros((gate_v.shape[0], padded - hidden_units), BF16)
        up_v[:, hidden_units:] = jnp.zeros((gate_v.shape[0], padded - hidden_units), BF16)
        down_v[hidden_units:, :] = jnp.zeros((padded - hidden_units, down_v.shape[1]), BF16)
    widened = tokens_ref[...].astype(F32)
    scaled = (widened * gain_ref[...].astype(F32)).astype(BF16)
    rows = widened.shape[0]
    stat[me] = jnp.broadcast_to(jnp.sum(widened * widened, axis=1, keepdims=True), (rows, LANES))
    greet(n_kv, n_tp)
    share(stat, stat_s, stat_r, "kv", n_kv)
    loads[0].wait()
    loads[1].wait()

    def partial(j):
        columns = pl.ds(pl.multiple_of(j * width, LANES), width)
        return (
            jnp.dot(scaled, gate_v[:, columns], preferred_element_type=F32),
            jnp.dot(scaled, up_v[:, columns], preferred_element_type=F32),
        )

    def spread(k, carry):
        peer = lax.rem(me + k, n_kv)
        gate_part, up_part = partial(peer)
        send[peer, :, :width] = gate_part.astype(BF16)
        send[peer, :, width:] = up_part.astype(BF16)
        remote(send.at[peer], recv.at[me], rs_s.at[peer], rs_r.at[me], "kv", peer).start()
        return carry

    lax.fori_loop(1, n_kv, spread, 0)
    own = jnp.concatenate(partial(me), axis=1)
    collect(stat, stat_s, stat_r, "kv", n_kv)
    factor = lax.rsqrt(total_over(stat, n_kv)[:, :1] / d_total + EPSILON)

    def gather(k, so_far):
        peer = lax.rem(me + k, n_kv)
        remote(send.at[peer], recv.at[peer], rs_s.at[peer], rs_r.at[peer], "kv", peer).wait_recv()
        return so_far + recv[peer].astype(F32)

    both = lax.fori_loop(1, n_kv, gather, own)
    gate_value = factor * both[:, :width]
    up_value = factor * both[:, width:]
    hid[me] = (gate_value / (1.0 + jnp.exp(-gate_value)) * up_value).astype(BF16)
    share(hid, ag_s, ag_r, "kv", n_kv)
    loads[2].wait()

    def down(j):
        return jnp.dot(
            hid[j], down_v[pl.ds(pl.multiple_of(j * width, LANES), width), :],
            preferred_element_type=F32,
        )

    def further(k, so_far):
        peer = lax.rem(me + k, n_kv)
        shared_from(hid, ag_s, ag_r, "kv", peer)
        return so_far + down(peer)

    part = lax.fori_loop(1, n_kv, further, down(me))
    summed = across_tp(part, tp_buf, tp_s, tp_r, n_tp)
    out_ref[...] = (widened + 0.5 * summed).astype(BF16)

    def sent(k, carry):
        peer = lax.rem(me + k, n_kv)
        remote(send.at[peer], recv.at[me], rs_s.at[peer], rs_r.at[me], "kv", peer).wait_send()
        return carry

    lax.fori_loop(1, n_kv, sent, 0)
    drain(stat, stat_s, stat_r, "kv", n_kv)
    drain(hid, ag_s, ag_r, "kv", n_kv)
    drain(tp_buf, tp_s, tp_r, "tp", n_tp)


VM = pl.BlockSpec(memory_space=pltpu.VMEM)
ANY = pl.BlockSpec(memory_space=pl.ANY)
DMA = pltpu.SemaphoreType.DMA


def feed_forward(tokens, gain, gate, up, down, identity):
    n_kv, n_tp = lax.axis_size("kv"), lax.axis_size("tp")
    rows, features = tokens.shape
    hidden_units = gate.shape[1]
    width = chunk_width(hidden_units, n_kv)
    padded = width * n_kv
    return pl.pallas_call(
        functools.partial(feed_kernel, n_kv, n_tp, width, float(features * n_kv)),
        out_shape=jax.ShapeDtypeStruct((rows, features), BF16),
        in_specs=[VM, VM, ANY, ANY, ANY],
        out_specs=VM,
        scratch_shapes=[
            pltpu.VMEM((features, padded), BF16),
            pltpu.VMEM((features, padded), BF16),
            pltpu.VMEM((padded, features), BF16),
            pltpu.VMEM((n_kv, rows, LANES), F32),
            pltpu.VMEM((n_kv, rows, 2 * width), BF16),
            pltpu.VMEM((n_kv, rows, 2 * width), BF16),
            pltpu.VMEM((n_kv, rows, width), BF16),
            pltpu.VMEM((n_tp, rows, features), BF16),
            DMA((3,)),
            DMA((n_kv,)), DMA((n_kv,)),
            DMA((n_kv,)), DMA((n_kv,)),
            DMA((n_kv,)), DMA((n_kv,)),
            DMA((n_tp,)), DMA((n_tp,)),
        ],
        compiler_params=pltpu.CompilerParams(
            collective_id=identity, has_side_effects=True, vmem_limit_bytes=32 << 20
        ),
        name=f"feed_{identity}",
    )(tokens, gain.reshape(1, features), gate, up, down)


def project_kernel(
    n_kv, n_tp, width, d_total,
    tokens_ref, gain_ref, query_hbm, key_hbm, value_hbm, forget_ref, bias_ref, out_ref, gates_ref,
    w_v, stat, send, recv, mine,
    w_sems, stat_s, stat_r, rs_s, rs_r, ag_s, ag_r,
):
    me = lax.axis_index("kv")
    each = query_hbm.shape[1]
    loads = [
        pltpu.make_async_copy(part, w_v.at[:, pl.ds(i * each, each)], w_sems.at[i])
        for i, part in enumerate((query_hbm, key_hbm, value_hbm))
    ]
    for load in loads:
        load.start()
    padded = w_v.shape[1]
    if padded > 3 * each:
        w_v[:, 3 * each :] = jnp.zeros((w_v.shape[0], padded - 3 * each), BF16)
    widened = tokens_ref[...].astype(F32)
    scaled = (widened * gain_ref[...].astype(F32)).astype(BF16)
    rows, features = widened.shape
    heads = forget_ref.shape[1]
    forget_rows = forget_ref[pl.ds(pl.multiple_of(me * features, features), features), :]
    stat[me, 0] = jnp.broadcast_to(jnp.sum(widened * widened, axis=1, keepdims=True), (rows, LANES))
    stat[me, 1] = jnp.zeros((rows, LANES), F32)
    stat[me, 1, :, :heads] = jnp.dot(scaled, forget_rows, preferred_element_type=F32)
    greet(n_kv, 1)
    share(stat, stat_s, stat_r, "kv", n_kv)
    for load in loads:
        load.wait()

    def partial(j):
        columns = pl.ds(pl.multiple_of(j * width, LANES), width)
        return jnp.dot(scaled, w_v[:, columns], preferred_element_type=F32)

    def spread(k, carry):
        peer = lax.rem(me + k, n_kv)
        send[peer] = partial(peer).astype(send.dtype)
        remote(send.at[peer], recv.at[me], rs_s.at[peer], rs_r.at[me], "kv", peer).start()
        return carry

    lax.fori_loop(1, n_kv, spread, 0)
    own = partial(me)
    collect(stat, stat_s, stat_r, "kv", n_kv)
    stats = total_over(stat, n_kv)
    factor = lax.rsqrt(stats[0][:, :1] / d_total + EPSILON)
    logits = factor * stats[1][:, :heads] + bias_ref[...]
    gates_ref[...] = jnp.minimum(logits, 0.0) - jnp.log1p(jnp.exp(-jnp.abs(logits)))

    def gather(k, so_far):
        peer = lax.rem(me + k, n_kv)
        remote(send.at[peer], recv.at[peer], rs_s.at[peer], rs_r.at[peer], "kv", peer).wait_recv()
        return so_far + recv[peer].astype(F32)

    mine[me] = (factor * lax.fori_loop(1, n_kv, gather, own)).astype(BF16)
    share(mine, ag_s, ag_r, "kv", n_kv)
    collect(mine, ag_s, ag_r, "kv", n_kv)
    for j in range(-(-3 * each // width)):
        out_ref[:, j * width : (j + 1) * width] = mine[j]

    def sent(k, carry):
        peer = lax.rem(me + k, n_kv)
        remote(send.at[peer], recv.at[me], rs_s.at[peer], rs_r.at[me], "kv", peer).wait_send()
        return carry

    lax.fori_loop(1, n_kv, sent, 0)
    drain(stat, stat_s, stat_r, "kv", n_kv)
    drain(mine, ag_s, ag_r, "kv", n_kv)


def project(tokens, gain, query, key, value, forget, bias):
    n_kv, n_tp = lax.axis_size("kv"), lax.axis_size("tp")
    rows, features = tokens.shape
    total = 3 * query.shape[1]
    width = chunk_width(total, n_kv)
    padded = width * n_kv
    columns = width * (-(-total // width))
    heads = forget.shape[1]
    return pl.pallas_call(
        functools.partial(project_kernel, n_kv, n_tp, width, float(features * n_kv)),
        out_shape=(
            jax.ShapeDtypeStruct((rows, columns), BF16),
            jax.ShapeDtypeStruct((rows, heads), F32),
        ),
        in_specs=[VM, VM, ANY, ANY, ANY, VM, VM],
        out_specs=(VM, VM),
        scratch_shapes=[
            pltpu.VMEM((features, padded), BF16),
            pltpu.VMEM((n_kv, 2, rows, LANES), F32),
            pltpu.VMEM((n_kv, rows, width), F32),
            pltpu.VMEM((n_kv, rows, width), F32),
            pltpu.VMEM((n_kv, rows, width), BF16),
            DMA((3,)),
            DMA((n_kv,)), DMA((n_kv,)),
            DMA((n_kv,)), DMA((n_kv,)),
            DMA((n_kv,)), DMA((n_kv,)),
        ],
        compiler_params=pltpu.CompilerParams(
            collective_id=1, has_side_effects=True, vmem_limit_bytes=24 << 20
        ),
        name="project",
    )(tokens, gain.reshape(1, features), query, key, value, forget, bias.reshape(1, heads))


def attend_kernel(inverse, q_ref, bias_ref, k_ref, v_ref, num_ref, top_ref, den_ref):
    heads = q_ref.shape[1]
    spots = k_ref.shape[1]
    head_of = lax.broadcasted_iota(jnp.int32, (heads, spots), 0)
    spot_of = lax.broadcasted_iota(jnp.int32, (heads, spots), 1)
    same = lax.rem(spot_of, heads) == head_of
    for i in range(q_ref.shape[0]):
        scores = lax.dot_general(
            q_ref[i], k_ref[i], (((1,), (1,)), ((), ())), preferred_element_type=F32
        )
        scores = jnp.where(same, scores * inverse + bias_ref[i], -jnp.inf)
        top = jnp.max(scores, axis=1, keepdims=True)
        weights = jnp.exp(scores - top).astype(BF16)
        den = jnp.sum(weights.astype(F32), axis=1, keepdims=True)
        num_ref[i] = jnp.dot(weights, v_ref[i], preferred_element_type=F32)
        top_ref[i] = jnp.broadcast_to(top, (heads, LANES))
        den_ref[i] = jnp.broadcast_to(den, (heads, LANES))


def attend(query, bias, keys, values):
    count, heads, size = query.shape
    spots = keys.shape[1]
    group = 2 if count % 2 == 0 else 1
    at = lambda b: (b, 0, 0)
    result = jax.ShapeDtypeStruct((count, heads, size), F32)
    stat = jax.ShapeDtypeStruct((count, heads, LANES), F32)
    return pl.pallas_call(
        functools.partial(attend_kernel, size ** (-0.5)),
        grid=(count // group,),
        out_shape=(result, stat, stat),
        in_specs=[
            pl.BlockSpec((group, heads, size), at),
            pl.BlockSpec((group, 1, spots), at),
            pl.BlockSpec((group, spots, size), at),
            pl.BlockSpec((group, spots, size), at),
        ],
        out_specs=(
            pl.BlockSpec((group, heads, size), at),
            pl.BlockSpec((group, heads, LANES), at),
            pl.BlockSpec((group, heads, LANES), at),
        ),
        compiler_params=pltpu.CompilerParams(vmem_limit_bytes=32 << 20),
        name="attend",
    )(query, bias, keys, values)


def merge_kernel(
    n_kv, n_tp, part_count, inverse,
    tokens_ref, num_ref, top_ref, den_ref, q_ref, k_ref, v_ref, gate_ref, w_ref, out_ref,
    send, recv, att, tp_buf,
    rs_s, rs_r, ag_s, ag_r, tp_s, tp_r,
):
    me = lax.axis_index("kv")
    count, heads = num_ref.shape[0], num_ref.shape[1]
    for i in range(n_kv):
        low, high = i * part_count, min((i + 1) * part_count, count)
        if high - low < part_count:
            send[i] = jnp.zeros(send.shape[1:], F32)
        if high > low:
            send[i, 0, : high - low] = num_ref[low:high]
            send[i, 1, : high - low] = top_ref[low:high]
            send[i, 2, : high - low] = den_ref[low:high]
    greet(n_kv, n_tp)

    def spread(k, carry):
        peer = lax.rem(me + k, n_kv)
        remote(send.at[peer], recv.at[me], rs_s.at[peer], rs_r.at[me], "kv", peer).start()
        return carry

    lax.fori_loop(1, n_kv, spread, 0)
    mine = pl.ds(me * part_count, part_count)
    query = q_ref[mine].astype(F32)
    own = jnp.sum(query * k_ref[mine].astype(F32), axis=2, keepdims=True) * inverse
    log_gate = gate_ref[mine]

    def gather(k, so_far):
        peer = lax.rem(me + k, n_kv)
        remote(send.at[peer], recv.at[peer], rs_s.at[peer], rs_r.at[peer], "kv", peer).wait_recv()
        num, top, den = so_far
        high = jnp.maximum(top, recv[peer, 1])
        old, new = jnp.exp(top - high), jnp.exp(recv[peer, 1] - high)
        return num * old + recv[peer, 0] * new, high, den * old + recv[peer, 2] * new

    num, top, den = lax.fori_loop(1, n_kv, gather, (send[me, 0], send[me, 1], send[me, 2]))
    top = top + log_gate
    ceiling = jnp.maximum(top, own)
    cache_scale, own_scale = jnp.exp(top - ceiling), jnp.exp(own - ceiling)
    attended = (num * cache_scale + own_scale * v_ref[mine].astype(F32)) / (
        den * cache_scale + own_scale
    )
    att[me] = attended.astype(BF16).astype(F32)
    share(att, ag_s, ag_r, "kv", n_kv)
    collect(att, ag_s, ag_r, "kv", n_kv)
    whole = att[...].reshape((n_kv * part_count, heads, LANES))[:count]
    size = LANES
    part = jnp.zeros((count, w_ref.shape[1]), F32)
    for h in range(heads):
        part += jnp.dot(
            whole[:, h, :].astype(BF16), w_ref[h * size : (h + 1) * size, :],
            preferred_element_type=F32,
        )
    summed = across_tp(part, tp_buf, tp_s, tp_r, n_tp)
    out_ref[...] = (tokens_ref[...].astype(F32) + summed).astype(BF16)

    def sent(k, carry):
        peer = lax.rem(me + k, n_kv)
        remote(send.at[peer], recv.at[me], rs_s.at[peer], rs_r.at[me], "kv", peer).wait_send()
        return carry

    lax.fori_loop(1, n_kv, sent, 0)
    drain(att, ag_s, ag_r, "kv", n_kv)
    drain(tp_buf, tp_s, tp_r, "tp", n_tp)


def merge(tokens, num, top, den, query, key, value, log_gate, out_weight):
    n_kv, n_tp = lax.axis_size("kv"), lax.axis_size("tp")
    rows, features = tokens.shape
    count, heads, size = num.shape
    part_count = -(-count // n_kv)
    pad = ((0, part_count * n_kv - count), (0, 0), (0, 0))
    query, key, value = (jnp.pad(x, pad) for x in (query, key, value))
    log_gate = jnp.pad(jnp.broadcast_to(log_gate[:, :, None], (count, heads, LANES)), pad)
    return pl.pallas_call(
        functools.partial(merge_kernel, n_kv, n_tp, part_count, size ** (-0.5)),
        out_shape=jax.ShapeDtypeStruct((rows, features), BF16),
        in_specs=[VM] * 9,
        out_specs=VM,
        scratch_shapes=[
            pltpu.VMEM((n_kv, 3, part_count, heads, LANES), F32),
            pltpu.VMEM((n_kv, 3, part_count, heads, LANES), F32),
            pltpu.VMEM((n_kv, part_count, heads, LANES), F32),
            pltpu.VMEM((n_tp, rows, features), BF16),
            DMA((n_kv,)), DMA((n_kv,)),
            DMA((n_kv,)), DMA((n_kv,)),
            DMA((n_tp,)), DMA((n_tp,)),
        ],
        compiler_params=pltpu.CompilerParams(
            collective_id=2, has_side_effects=True, vmem_limit_bytes=24 << 20
        ),
        name="merge",
    )(tokens, num, top, den, query, key, value, log_gate, out_weight)


def on_device(
    tokens,
    gain_first,
    gate_first,
    up_first,
    down_first,
    gain_mixer,
    query_weight,
    key_weight,
    value_weight,
    forget_weight,
    forget_bias,
    key_cache,
    value_cache,
    forget_sum,
    out_weight,
    gain_second,
    gate_second,
    up_second,
    down_second,
):
    count, spots, heads, size = key_cache.shape
    bias = forget_sum.transpose(0, 2, 1).reshape(count, 1, spots * heads)
    first_out = feed_forward(tokens, gain_first, gate_first, up_first, down_first, 0)
    projected, all_gates = project(
        first_out, gain_mixer, query_weight, key_weight, value_weight, forget_weight, forget_bias
    )
    each = heads * size
    query, new_key, new_value = (
        projected[:, i * each : (i + 1) * each].reshape(count, heads, size) for i in range(3)
    )
    log_gate = lax.dynamic_slice_in_dim(all_gates, lax.axis_index("tp") * heads, heads, 1)
    num, top, den = attend(
        query,
        bias,
        key_cache.reshape(count, spots * heads, size),
        value_cache.reshape(count, spots * heads, size),
    )
    mixed = merge(first_out, num, top, den, query, new_key, new_value, log_gate, out_weight)
    return feed_forward(mixed, gain_second, gate_second, up_second, down_second, 3)


def solution(mesh):
    in_specs = (
        P(None, "kv"),
        P("kv"),
        P("kv", "tp"),
        P("kv", "tp"),
        P("tp", "kv"),
        P("kv"),
        P("kv", "tp"),
        P("kv", "tp"),
        P("kv", "tp"),
        P(),
        P(),
        P(None, "kv", "tp", None),
        P(None, "kv", "tp", None),
        P(None, "tp", "kv"),
        P("tp", "kv"),
        P("kv"),
        P("kv", "tp"),
        P("kv", "tp"),
        P("tp", "kv"),
    )
    return jax.shard_map(
        on_device, mesh=mesh, in_specs=in_specs, out_specs=P(None, "kv"), check_vma=False
    )
```
